32 devices in a mesh: sp: 8 (over z, x), tp: 4 (over y, core).
Axes of the slice: x: 2, y: 2, z: 4, core: 2. Of those that a mesh axis runs over, the one named last changes fastest.
Arguments:
- queries: bfloat16 [8192, 1024], P('sp', 'tp'), may hold values from -75 to 75
- key_rows: bfloat16 [8192, 1024], P('sp', 'tp'), may hold values from -4 to 4
- value_rows: bfloat16 [8192, 1024], P('sp', 'tp'), may hold values from -6 to 6
- cum_gate: float32 [16, 8192], P('tp'), may hold values from -1172 to 0, as said below
- residual: bfloat16 [8192, 2048], P(('sp', 'tp')), may hold values from -6 to 6
- out_weight: bfloat16 [1024, 2048], replicated, may hold values from -0.1875 to 0.1875
- gain_mix: float32 [2048], replicated, may hold values from 0.1 to 1.9
- gain_pre: float32 [2048], replicated, may hold values from 0.1 to 1.9
- gain_post: float32 [2048], replicated, may hold values from 0.1 to 1.9
- route_ids: int32 [8192, 2], P(('sp', 'tp')), may hold values from 0 to 31, all different within a row; in each aligned block of 256 rows (0 to 255, 256 to 511, ...) at most 22 rows name the same one
- route_weight: float32 [8192, 2], P(('sp', 'tp')), may hold values from 0.2 to 1
- w_gate: bfloat16 [32, 2048, 512], P(('sp', 'tp')), may hold values from -0.125 to 0.125
- w_up: bfloat16 [32, 2048, 512], P(('sp', 'tp')), may hold values from -0.125 to 0.125
- w_down: bfloat16 [32, 512, 2048], P(('sp', 'tp')), may hold values from -0.25 to 0.25
Outputs:
- layer_out: bfloat16 [8192, 2048], P(('sp', 'tp'))
The draws below stay inside these ranges and needn't reach their ends.
Inputs may be any that keep to these rules, and one draw needn't show every extreme that they name: `route_ids`: each row names 2 different experts; in the rows of one device no expert is named more than 22 times, a bound that some block reaches. `cum_gate`: along the positions each head's values never rise.
All inputs are finite; a program needn't handle non-finite values.
Results may differ from the reference program's by a relative error of at most 0.018.
Values may be sent and summed in bfloat16 or wider, within the bound.
A program may use at most 128 MiB of HBM per device.

```python
import math
import jax
import jax.numpy as jnp
import numpy as np
from jax import lax

D = 2048
ATTENTION_HEADS = 16
HEAD_DIM = 64
FF = 512
TOP = 2
TOK_DEV = 1024
TOKEN_COUNT = 8192
ROWS = 256
EXPERTS = 32
CAP = 22
N_SP = 8
N_TP = 4


def draw_queries(key, part):
    sample = jax.random.normal(jax.random.fold_in(key, 1), (TOKEN_COUNT, ATTENTION_HEADS * HEAD_DIM), jnp.float32)
    return jnp.clip(sample, -4.0, 4.0).astype(jnp.bfloat16)


def draw_key_rows(key, part):
    sample = jax.random.normal(jax.random.fold_in(key, 2), (TOKEN_COUNT, ATTENTION_HEADS * HEAD_DIM), jnp.float32)
    return jnp.clip(sample, -4.0, 4.0).astype(jnp.bfloat16)


def draw_cum_gate(key, part):
    key_o, key_s, key_f, key_r, key_b, random_key_position, random_key_log = jax.random.split(jax.random.fold_in(key, 5), 7)
    shuffle = jax.random.permutation(key_o, ATTENTION_HEADS)
    slow_head = shuffle < ATTENTION_HEADS // 2
    slow_total = jax.random.uniform(key_s, (ATTENTION_HEADS,), jnp.float32, 0.4, 1.0)
    fast_rate = jnp.exp(jax.random.uniform(key_f, (ATTENTION_HEADS,), jnp.float32, -4.6, -3.4))
    step_rate = jnp.where(slow_head, slow_total / TOKEN_COUNT, fast_rate)
    blocks = TOKEN_COUNT // TOK_DEV
    roughness = jnp.exp(jax.random.uniform(key_r, (ATTENTION_HEADS, blocks, TOK_DEV), jnp.float32, -0.7, 0.7))
    block_factor = jnp.exp(jax.random.uniform(key_b, (ATTENTION_HEADS, blocks, 1), jnp.float32, -0.7, 0.7))
    logarithm_steps = step_rate[:, None] * (roughness * block_factor).reshape(ATTENTION_HEADS, TOKEN_COUNT)
    spike_position = jax.random.randint(random_key_position, (ATTENTION_HEADS, 2), 0, TOKEN_COUNT)
    spike_decay = -jnp.log(1.0 - jax.random.uniform(random_key_log, (ATTENTION_HEADS, 2), jnp.float32, 0.2, 0.45))
    index_of_head = jnp.broadcast_to(lax.iota(jnp.int32, ATTENTION_HEADS)[:, None], (ATTENTION_HEADS, 2))
    logarithm_steps = logarithm_steps.at[index_of_head, spike_position].add(spike_decay)
    return -jnp.cumsum(logarithm_steps, axis=1)


def steps_of(own_key, extent, cuts, least, high):
    def one(position, parts):
        draws = jax.random.uniform(jax.random.fold_in(jax.random.fold_in(own_key, 6), position), (parts,), jnp.float32, least / len(cuts), high / len(cuts))
        return jnp.repeat(jnp.exp(draws), extent[position] // parts).reshape((-1,) + (1,) * (len(extent) - position - 1))

    level = one(*cuts[0])
    for cut in cuts[1:]:
        level = level * one(*cut)
    return level


def shared_out(own_key, own, number, rows, number_of, top, bound, skew):
    ranking = jax.random.permutation(own_key, number_of)
    heavy_load, ordinary = shares(number_of, rows * top, bound, skew, True), shares(number_of, rows * top, bound, skew, False)
    places = jnp.arange(number_of)

    def named(lengths, offset_by):
        used = int((lengths > 0).sum())
        fixed = max(1, used // 4)
        passed = fixed + (places - fixed + offset_by * (used - fixed)) % max(1, number_of - fixed)
        return jnp.zeros((number_of,), jnp.int32).at[ranking[jnp.where(places < fixed, places, passed)]].set(jnp.asarray(lengths, jnp.int32))

    lengths = jnp.where(number % 4 == 0, named(heavy_load, number // 4), named(ordinary, number - number // 4 - 1))
    mixed = jax.random.permutation(jax.random.fold_in(own, 3), number_of)
    source_of, taker = mixed[0:number_of // 2 * 2:2], mixed[1:number_of // 2 * 2:2]
    slack = jnp.minimum(lengths[source_of] - 1, bound - lengths[taker]) // 2
    slack = jnp.where((source_of == ranking[0]) | (taker == ranking[0]) | (lengths[taker] == 0), 0, jnp.maximum(slack, 0))
    passed = jax.random.randint(jax.random.fold_in(own, 4), (number_of // 2,), 0, 1 << 20) % (slack + 1)
    lengths = lengths.at[source_of].add(-passed).at[taker].add(passed)
    labels = jnp.searchsorted(jnp.cumsum(lengths), jnp.arange(rows * top), side="right").astype(jnp.int32)
    grid = labels.reshape(top, rows).T
    grid = grid[jax.random.permutation(jax.random.fold_in(own, 1), rows)]
    offset_by = jax.random.randint(jax.random.fold_in(own, 2), (rows, 1), 0, top)
    return jnp.take_along_axis(grid, (jnp.arange(top)[None, :] + offset_by) % top, axis=1)


def shares(count, total, reach, skew, full):
    portions = [(1 << 20) // math.isqrt(rank ** skew) + 1 for rank in range(1, count + 1)]
    largest = reach if full else min(reach, max(-(-total // count), total * portions[0] // sum(portions)))
    least = 1 if total - largest >= count - 1 else 0
    holding, spare = [largest] + [least] * (count - 1), total - largest - least * (count - 1)
    while spare > 0:
        free = [i for i in range(1, count) if holding[i] < largest] or [i for i in range(1, count) if holding[i] < reach]
        pool, remaining = sum([portions[i] for i in free]), spare
        for i in free:
            more = min(reach - holding[i], max(1, remaining * portions[i] // pool), spare)
            holding[i] = holding[i] + more
            spare = spare - more
    return np.array(holding)


def scatter_about(own_key, dims, deviation, reach, shards=(), kind=jnp.bfloat16):
    values = jax.random.normal(own_key, dims, jnp.float32) * deviation
    if len(shards) > 0:
        values = steps_of(own_key, dims, shards, -0.22, 0.18) * values
    return jnp.clip(values, min=-reach, max=reach).astype(kind)


def setup_inputs(seed: int = 0) -> dict:
    keys = jax.random.split(jax.random.key(seed), 15)
    queries = draw_queries(jax.random.fold_in(keys[14], 71), 0)
    key_rows = draw_key_rows(jax.random.fold_in(keys[14], 71), 0)
    value_rows = scatter_about(keys[2], (TOKEN_COUNT, ATTENTION_HEADS * HEAD_DIM), 1.0, 6.0, ((0, 8), (1, 4)))
    cum_gate = draw_cum_gate(jax.random.fold_in(keys[14], 71), 0)
    residual = scatter_about(keys[4], (TOKEN_COUNT, D), 1.0, 6.0, ((0, 32),))
    out_weight = scatter_about(keys[5], (ATTENTION_HEADS * HEAD_DIM, D), (ATTENTION_HEADS * HEAD_DIM) ** -0.5, 0.1875)
    gain_mix = jnp.clip(1.0 + 0.18 * jax.random.normal(keys[6], (D,), jnp.float32), 0.1, 1.9)
    gain_pre = jnp.clip(1.0 + 0.18 * jax.random.normal(keys[7], (D,), jnp.float32), 0.1, 1.9)
    gain_post = jnp.clip(1.0 + 0.18 * jax.random.normal(keys[8], (D,), jnp.float32), 0.1, 1.9)
    route_ids_keys = jax.random.split(jax.random.fold_in(keys[9], 1), TOKEN_COUNT // ROWS)
    route_ids_turns = jax.random.permutation(jax.random.fold_in(keys[9], 3), TOKEN_COUNT // ROWS)
    route_ids = jax.vmap(lambda own, number: shared_out(jax.random.fold_in(keys[9], 2), own, number, ROWS, EXPERTS, TOP, CAP, 1))(route_ids_keys, route_ids_turns).reshape((TOKEN_COUNT, TOP))
    route_weight = jnp.clip(jnp.exp(math.log(1.0) - 1.609438 * jax.random.uniform(keys[10], (TOKEN_COUNT, TOP), jnp.float32) ** steps_of(keys[10], (TOKEN_COUNT, TOP), ((0, 32),), -0.2, 0.2)), 0.2, 1.0)
    w_gate = scatter_about(keys[11], (EXPERTS, D, FF), D ** -0.5, 0.125, ((0, 32),))
    w_up = scatter_about(keys[12], (EXPERTS, D, FF), D ** -0.5, 0.125, ((0, 32),))
    w_down = scatter_about(keys[13], (EXPERTS, FF, D), FF ** -0.5, 0.25, ((0, 32),))
    return {"queries": queries, "key_rows": key_rows, "value_rows": value_rows, "cum_gate": cum_gate, "residual": residual, "out_weight": out_weight, "gain_mix": gain_mix, "gain_pre": gain_pre, "gain_post": gain_post, "route_ids": route_ids, "route_weight": route_weight, "w_gate": w_gate, "w_up": w_up, "w_down": w_down}


NORM_EPS = 1e-06
MASKED = -1e+30

def rms_scale(rows, gain):
    mean_sq = lax.optimization_barrier(jnp.mean(rows * rows, axis=-1, keepdims=True))
    return rows * lax.rsqrt(mean_sq + NORM_EPS) * gain

def attend(running, queries, gate_q, q_start, key_part, value_part, gate_k, k_start):
    row_peak, row_total, weighted = running
    scores = jnp.einsum('qhd,khd->hqk', queries.astype(jnp.float32), key_part.astype(jnp.float32)) * HEAD_DIM ** (-0.5)
    scores = scores + gate_q[:, :, None] - gate_k[:, None, :]
    query_pos = q_start + lax.iota(jnp.int32, queries.shape[0])
    key_pos = k_start + lax.iota(jnp.int32, key_part.shape[0])
    allowed = (key_pos[None, :] <= query_pos[:, None])[None]
    scores = jnp.where(allowed, scores, MASKED)
    new_peak = jnp.maximum(row_peak, lax.optimization_barrier(jnp.max(scores, axis=-1)))
    unnorm = jnp.where(allowed, jnp.exp(scores - new_peak[..., None]), 0.0)
    rescale = jnp.exp(row_peak - new_peak)
    row_total = row_total * rescale + lax.optimization_barrier(jnp.sum(unnorm, axis=-1))
    probs = lax.optimization_barrier(unnorm.astype(jnp.bfloat16)).astype(jnp.float32)
    weighted = weighted * rescale.T[:, :, None] + jnp.einsum('hqk,khd->qhd', probs, value_part.astype(jnp.float32))
    return (new_peak, row_total, weighted)

def attention(queries, key_rows, value_rows, cum_gate):
    query_heads = queries.reshape(TOKEN_COUNT, ATTENTION_HEADS, HEAD_DIM)
    key_heads = key_rows.reshape(TOKEN_COUNT, ATTENTION_HEADS, HEAD_DIM)
    value_heads = value_rows.reshape(TOKEN_COUNT, ATTENTION_HEADS, HEAD_DIM)

    def one_block(block_index):
        q_start = block_index * TOK_DEV
        query_block = lax.dynamic_slice_in_dim(query_heads, q_start, TOK_DEV, 0)
        gate_q = lax.dynamic_slice_in_dim(cum_gate, q_start, TOK_DEV, 1)
        initial = (jnp.full((ATTENTION_HEADS, TOK_DEV), MASKED, jnp.float32), jnp.zeros((ATTENTION_HEADS, TOK_DEV), jnp.float32), jnp.zeros((TOK_DEV, ATTENTION_HEADS, HEAD_DIM), jnp.float32))

        def key_block(other, running):
            k_start = (other * TOK_DEV).astype(jnp.int32)
            return attend(running, query_block, gate_q, q_start, lax.dynamic_slice_in_dim(key_heads, k_start, TOK_DEV, 0), lax.dynamic_slice_in_dim(value_heads, k_start, TOK_DEV, 0), lax.dynamic_slice_in_dim(cum_gate, k_start, TOK_DEV, 1), k_start)
        row_peak, row_total, weighted = lax.fori_loop(jnp.int32(0), block_index + 1, key_block, initial)
        return (weighted / row_total.T[:, :, None]).astype(jnp.bfloat16)
    blocks = lax.map(one_block, jnp.arange(N_SP, dtype=jnp.int32))
    return blocks.reshape(TOKEN_COUNT, ATTENTION_HEADS * HEAD_DIM)

def route_experts(normed, route_ids, route_weight, w_gate, w_up, w_down):
    sources = N_SP * N_TP
    flat_ids = route_ids.reshape(sources, ROWS * TOP)
    onehot = (flat_ids[:, :, None] == jnp.arange(EXPERTS, dtype=jnp.int32)[None, None, :]).astype(jnp.int32)
    slot_rank = (lax.optimization_barrier(jnp.sum(jnp.cumsum(onehot, axis=1) * onehot, axis=2)) - 1).astype(jnp.int32)
    slot_index = flat_ids * (sources * CAP) + jnp.arange(sources, dtype=jnp.int32)[:, None] * CAP + slot_rank
    slot_index = slot_index.reshape(-1).astype(jnp.int32)
    token_index = jnp.arange(TOKEN_COUNT * TOP, dtype=jnp.int32) // TOP
    slot_count = EXPERTS * sources * CAP
    source_row = jnp.zeros((slot_count,), jnp.int32).at[slot_index].set(token_index)
    slot_weight = jnp.zeros((slot_count,), jnp.float32).at[slot_index].set(route_weight.reshape(-1))

    def one_expert(summed, expert):
        offset = (expert * sources * CAP).astype(jnp.int32)
        picked_rows = lax.dynamic_slice_in_dim(source_row, offset, sources * CAP)
        weights = lax.dynamic_slice_in_dim(slot_weight, offset, sources * CAP)
        routed = normed[picked_rows]
        gate_act = jnp.dot(routed, w_gate[expert], preferred_element_type=jnp.float32)
        up_act = jnp.dot(routed, w_up[expert], preferred_element_type=jnp.float32)
        hidden = (jax.nn.silu(gate_act) * up_act).astype(jnp.bfloat16)
        result = jnp.dot(hidden, w_down[expert], preferred_element_type=jnp.float32).astype(jnp.bfloat16)
        summed = summed.at[picked_rows].add(weights[:, None] * result.astype(jnp.float32))
        return (summed, None)
    summed, _ = lax.scan(one_expert, jnp.zeros((TOKEN_COUNT, D), jnp.float32), jnp.arange(EXPERTS, dtype=jnp.int32))
    return summed

def reference(queries, key_rows, value_rows, cum_gate, residual, out_weight, gain_mix, gain_pre, gain_post, route_ids, route_weight, w_gate, w_up, w_down):
    attended = attention(queries, key_rows, value_rows, cum_gate)
    projected = jnp.dot(attended, out_weight, preferred_element_type=jnp.float32)
    stream = (residual.astype(jnp.float32) + rms_scale(projected, gain_mix)).astype(jnp.bfloat16)
    stream_wide = lax.optimization_barrier(stream).astype(jnp.float32)
    normed = rms_scale(stream_wide, gain_pre).astype(jnp.bfloat16)
    combined = route_experts(normed, route_ids, route_weight, w_gate, w_up, w_down)
    return (stream_wide + rms_scale(combined, gain_post)).astype(jnp.bfloat16)
```

```python
import functools
import math

import jax
import jax.numpy as jnp
from jax import lax
from jax.experimental import pallas as pl
from jax.experimental.pallas import tpu as pltpu
from jax.sharding import PartitionSpec as P

HEAD_DIM = 64
NORM_EPS = 1e-06
MASKED = -1e30


def rms_scale(rows, gain):
    mean_sq = jnp.mean(rows * rows, axis=-1, keepdims=True)
    return rows * lax.rsqrt(mean_sq + NORM_EPS) * gain


def bf16_parts(values):
    parts = []
    for _ in range(3):
        part = lax.reduce_precision(values, 8, 7)
        parts.append(part.astype(jnp.bfloat16))
        values = values - part
    return parts


def flash_kernel(q_ref, k_ref, v_ref, o_ref, *, block_q, block_k, tiles, rows_dev, sub, shares):
    tile = pl.program_id(0)
    rank = lax.rem(lax.axis_index("sp"), shares)
    queries = q_ref[...]

    def step(first, state, masked):
        peak, acc = state
        scores = lax.dot_general(
            queries,
            k_ref[pl.ds(first, block_k), :],
            (((1,), (1,)), ((), ())),
            preferred_element_type=jnp.float32,
        )
        if masked:
            row = lax.broadcasted_iota(jnp.int32, (block_q, 1), 0)
            pos = row // sub * rows_dev + rank * sub + row % sub
            key = lax.broadcasted_iota(jnp.int32, (1, block_k), 1)
            scores = jnp.where(key <= pos, scores, MASKED)
        new_peak = jnp.maximum(peak, jnp.max(scores, axis=1, keepdims=True))
        probs = jnp.exp(scores - new_peak).astype(jnp.bfloat16)
        acc = acc * jnp.exp(peak - new_peak) + jnp.dot(
            probs, v_ref[pl.ds(first, block_k), :], preferred_element_type=jnp.float32
        )
        return new_peak, acc

    state = (
        jnp.full((block_q, 1), MASKED, jnp.float32),
        jnp.zeros((block_q, v_ref.shape[1]), jnp.float32),
    )
    state = lax.fori_loop(
        0,
        tile,
        lambda i, state: step(pl.multiple_of(i * block_k, block_k), state, False),
        state,
    )
    _, acc = step(pl.multiple_of(tile * block_k, block_k), state, True)
    o_ref[...] = (acc[:, :HEAD_DIM] / acc[:, HEAD_DIM : HEAD_DIM + 1]).astype(o_ref.dtype)


def flash(q_aug, k_aug, v_aug, rows_dev, sub, shares, block_q):
    rows = q_aug.shape[0]
    tiles = rows // block_q
    body = functools.partial(
        flash_kernel,
        block_q=block_q,
        block_k=block_q * shares,
        tiles=tiles,
        rows_dev=rows_dev,
        sub=sub,
        shares=shares,
    )
    whole = pl.BlockSpec(memory_space=pltpu.VMEM)
    return pl.pallas_call(
        body,
        grid=(tiles,),
        out_shape=jax.ShapeDtypeStruct((rows, HEAD_DIM), jnp.bfloat16),
        in_specs=[pl.BlockSpec((block_q, q_aug.shape[1]), lambda i: (i, 0)), whole, whole],
        out_specs=pl.BlockSpec((block_q, HEAD_DIM), lambda i: (i, 0)),
        compiler_params=pltpu.CompilerParams(vmem_limit_bytes=50 * 2**20),
        name="flash",
    )(q_aug, k_aug, v_aug)


def local(
    queries,
    key_rows,
    value_rows,
    cum_gate,
    residual,
    out_weight,
    gain_mix,
    gain_pre,
    gain_post,
    route_ids,
    route_weight,
    w_gate,
    w_up,
    w_down,
):
    tok_dev, feature_width = queries.shape
    local_heads = feature_width // HEAD_DIM
    n_sp, n_tp = lax.axis_size("sp"), lax.axis_size("tp")
    shares = n_sp // local_heads
    rows_dev = residual.shape[0]
    sub = rows_dev // shares
    chunk = n_tp * sub
    half = chunk // 2
    q_send = queries.reshape(n_tp, shares, sub, local_heads, HEAD_DIM).transpose(3, 1, 0, 2, 4)
    q_send = q_send.reshape(n_sp, chunk, HEAD_DIM)
    q_send = jnp.concatenate((q_send[:, :half], q_send[:, half:]), axis=2)
    kv_send = jnp.concatenate(
        (
            key_rows.reshape(tok_dev, local_heads, HEAD_DIM),
            value_rows.reshape(tok_dev, local_heads, HEAD_DIM),
        ),
        axis=2,
    ).transpose(1, 0, 2)
    kv_send = jnp.repeat(kv_send, shares, axis=0)
    sent = jnp.concatenate((kv_send, q_send), axis=1)
    got = lax.all_to_all(sent, "sp", split_axis=0, concat_axis=0, tiled=True)
    kv = got[:, :tok_dev].reshape(n_sp * tok_dev, 2 * HEAD_DIM)
    q_got = got[:, tok_dev:]
    q_got = jnp.concatenate((q_got[..., :HEAD_DIM], q_got[..., HEAD_DIM:]), axis=1)
    q_got = q_got.reshape(n_sp * chunk, HEAD_DIM) * jnp.bfloat16(HEAD_DIM**-0.5)

    me = lax.axis_index("sp")
    gate = lax.dynamic_index_in_dim(cum_gate, me // shares, 0, keepdims=False)
    gate_q = gate.reshape(n_sp * n_tp, shares, sub)
    gate_q = lax.dynamic_index_in_dim(gate_q, me % shares, 1, keepdims=False).reshape(-1)
    ones_q = jnp.ones((n_sp * chunk,), jnp.bfloat16)
    ones_k = jnp.ones((n_sp * tok_dev,), jnp.bfloat16)
    side_q = jnp.stack(bf16_parts(gate_q) + [ones_q] * 3, axis=1)
    side_k = jnp.stack([ones_k] * 3 + bf16_parts(-gate), axis=1)
    pad = ((0, 0), (0, HEAD_DIM - 6))
    q_aug = jnp.concatenate((q_got, jnp.pad(side_q, pad)), axis=1)
    k_aug = jnp.concatenate((kv[:, :HEAD_DIM], jnp.pad(side_k, pad)), axis=1)
    lane = lax.broadcasted_iota(jnp.int32, (n_sp * tok_dev, HEAD_DIM), 1)
    v_aug = jnp.concatenate((kv[:, HEAD_DIM:], (lane == 0).astype(jnp.bfloat16)), axis=1)
    out = flash(q_aug, k_aug, v_aug, rows_dev, sub, shares, chunk)

    out = out.reshape(n_sp * n_tp, sub, HEAD_DIM)
    out = jnp.concatenate((out[:, : sub // 2], out[:, sub // 2 :]), axis=2)
    heads = lax.all_to_all(out, ("sp", "tp"), split_axis=0, concat_axis=0, tiled=True)
    heads = heads.reshape(local_heads, shares, n_tp, sub // 2, 2, HEAD_DIM)
    head_rows = heads.transpose(1, 4, 3, 2, 0, 5).reshape(rows_dev, n_tp * feature_width)
    projected = jnp.dot(head_rows, out_weight, preferred_element_type=jnp.float32)
    stream = (residual.astype(jnp.float32) + rms_scale(projected, gain_mix)).astype(jnp.bfloat16)
    stream_wide = lax.optimization_barrier(stream).astype(jnp.float32)
    normed = rms_scale(stream_wide, gain_pre).astype(jnp.bfloat16)
    top_count = route_ids.shape[1]
    experts_all = n_sp * n_tp
    capacity = max(2, (4 * rows_dev * top_count + 3 * experts_all - 1) // (3 * experts_all))
    capacity = (capacity + 7) // 8 * 8
    flat_ids = route_ids.reshape(-1)
    item = lax.iota(jnp.int32, rows_dev * top_count)
    earlier = (item[None, :] < item[:, None]) & (flat_ids[None, :] == flat_ids[:, None])
    slot_index = flat_ids * capacity + jnp.sum(earlier.astype(jnp.int32), axis=1)
    slot_index = slot_index.reshape(rows_dev, top_count)
    slots_all = experts_all * capacity
    slot = lax.iota(jnp.int32, slots_all)
    place = sum((slot_index[:, k, None] == slot).astype(jnp.bfloat16) for k in range(top_count))
    outgoing = lax.dot_general(
        place, normed, (((0,), (0,)), ((), ())), preferred_element_type=jnp.float32
    ).astype(jnp.bfloat16)
    outgoing = outgoing.reshape(experts_all, capacity, -1)
    arrived = lax.all_to_all(outgoing, ("sp", "tp"), split_axis=0, concat_axis=0, tiled=True)
    flat_rows = arrived.reshape(slots_all, -1)
    gate_act = jnp.dot(flat_rows, w_gate[0], preferred_element_type=jnp.float32)
    up_act = jnp.dot(flat_rows, w_up[0], preferred_element_type=jnp.float32)
    hidden = (jax.nn.silu(gate_act) * up_act).astype(jnp.bfloat16)
    expert_out = jnp.dot(hidden, w_down[0], preferred_element_type=jnp.float32).astype(jnp.bfloat16)
    returned = lax.all_to_all(
        expert_out.reshape(experts_all, capacity, -1),
        ("sp", "tp"),
        split_axis=0,
        concat_axis=0,
        tiled=True,
    ).reshape(slots_all, -1)
    weigh = sum(
        jnp.where(slot_index[:, k, None] == slot, route_weight[:, k, None], 0.0)
        for k in range(top_count)
    )
    combined = sum(
        jnp.dot(part, returned, preferred_element_type=jnp.float32) for part in bf16_parts(weigh)
    )
    return (stream_wide + rms_scale(combined, gain_post)).astype(jnp.bfloat16)


def solution(mesh):
    return jax.shard_map(
        local,
        mesh=mesh,
        in_specs=(
            P("sp", "tp"),
            P("sp", "tp"),
            P("sp", "tp"),
            P("tp", None),
            P(("sp", "tp"), None),
            P(),
            P(),
            P(),
            P(),
            P(("sp", "tp"), None),
            P(("sp", "tp"), None),
            P(("sp", "tp"), None, None),
            P(("sp", "tp"), None, None),
            P(("sp", "tp"), None, None),
        ),
        out_specs=P(("sp", "tp"), None),
        check_vma=False,
    )
```

```python
import functools
import math

import jax
import jax.numpy as jnp
from jax import lax
from jax.experimental import pallas as pl
from jax.experimental.pallas import tpu as pltpu
from jax.sharding import PartitionSpec as P

HEAD_DIM = 64
NORM_EPS = 1e-06
MASKED = -1e30


def rms_scale(rows, gain):
    mean_sq = jnp.mean(rows * rows, axis=-1, keepdims=True)
    return rows * lax.rsqrt(mean_sq + NORM_EPS) * gain


def bf16_parts(values):
    parts = []
    for _ in range(3):
        part = lax.reduce_precision(values, 8, 7)
        parts.append(part.astype(jnp.bfloat16))
        values = values - part
    return parts


def pack_kernel(q_ref, k_ref, v_ref, one_ref, two_ref, *, shares, n_tp):
    tok_dev, width = q_ref.shape
    first = tok_dev - two_ref.shape[1]
    rows_dev = tok_dev // n_tp
    sub = rows_dev // shares
    for h in range(width // HEAD_DIM):
        cols = pl.ds(h * HEAD_DIM, HEAD_DIM)
        pairs = jnp.concatenate((k_ref[:, cols], v_ref[:, cols]), axis=1)
        for r in range(shares):
            dest = h * shares + r
            one_ref[dest, :first] = pairs[:first]
            two_ref[dest] = pairs[first:]
            for t in range(n_tp // 2):
                low, high = (
                    q_ref[pl.ds((t + step) * rows_dev + r * sub, sub), cols]
                    for step in (0, n_tp // 2)
                )
                one_ref[dest, pl.ds(first + t * sub, sub)] = jnp.concatenate((low, high), axis=1)


def pack(queries, key_rows, value_rows, first, shares, n_tp):
    tok_dev, width = queries.shape
    dests = width // HEAD_DIM * shares
    half = tok_dev // shares // 2
    shapes = [(dests, first + half, 2 * HEAD_DIM), (dests, tok_dev - first, 2 * HEAD_DIM)]
    return pl.pallas_call(
        functools.partial(pack_kernel, shares=shares, n_tp=n_tp),
        out_shape=[jax.ShapeDtypeStruct(shape, jnp.bfloat16) for shape in shapes],
        in_specs=[pl.BlockSpec(memory_space=pltpu.VMEM)] * 3,
        out_specs=[pl.BlockSpec(memory_space=pltpu.VMEM)] * 2,
        compiler_params=pltpu.CompilerParams(vmem_limit_bytes=32 * 2**20),
        name="pack",
    )(queries, key_rows, value_rows)


def assemble_kernel(in_ref, out_ref, *, shares, n_tp, local_heads):
    half = in_ref.shape[1]
    for t in range(n_tp):
        for h in range(0, local_heads, 2):
            for r in range(shares):
                left = in_ref[(h * shares + r) * n_tp + t]
                right = in_ref[((h + 1) * shares + r) * n_tp + t]
                for part in range(2):
                    cols = slice(part * HEAD_DIM, (part + 1) * HEAD_DIM)
                    out_ref[
                        pl.ds((2 * r + part) * half, half),
                        pl.ds((t * local_heads + h) * HEAD_DIM, 2 * HEAD_DIM),
                    ] = jnp.concatenate((left[:, cols], right[:, cols]), axis=1)


def assemble(heads, shares, n_tp, local_heads):
    shape = (2 * shares * heads.shape[1], n_tp * local_heads * HEAD_DIM)
    return pl.pallas_call(
        functools.partial(
            assemble_kernel, shares=shares, n_tp=n_tp, local_heads=local_heads
        ),
        out_shape=jax.ShapeDtypeStruct(shape, jnp.bfloat16),
        in_specs=[pl.BlockSpec(memory_space=pltpu.VMEM)],
        out_specs=pl.BlockSpec(memory_space=pltpu.VMEM),
        name="assemble",
    )(heads)


def flash_kernel(*refs, begun, span, shares, sub, rows_dev, n_tp):
    if begun:
        q_ref, kv_ref, side_q_ref, side_k_ref, state_ref, o_ref, k_aug, v_aug = refs
    else:
        q_ref, kv_ref, side_q_ref, side_k_ref, o_ref, k_aug, v_aug = refs
    lo, hi = span
    count = hi - lo
    tile = pl.program_id(0)
    rank = lax.rem(lax.axis_index("sp"), shares)

    @pl.when(tile == 0)
    def _():
        lane = lax.broadcasted_iota(jnp.int32, (count, 2 * HEAD_DIM), 1)

        def one(src, carry):
            kv = kv_ref[src, :count].astype(jnp.float32)
            side = side_k_ref[src, lo:hi].astype(jnp.float32)
            k_aug[src] = jnp.where(lane < HEAD_DIM, kv, side).astype(jnp.bfloat16)
            ones = (lane == 0).astype(jnp.float32)
            v_aug[src] = jnp.where(lane < HEAD_DIM, ones, kv).astype(jnp.bfloat16)
            return carry

        lax.fori_loop(0, kv_ref.shape[0], one, 0)

    packed = q_ref[0]
    queries = jnp.concatenate((packed[:, :HEAD_DIM], packed[:, HEAD_DIM:]), axis=0)
    queries = queries * jnp.bfloat16(HEAD_DIM**-0.5)
    queries = jnp.concatenate((queries, side_q_ref[:, HEAD_DIM:]), axis=1)
    rows = queries.shape[0]
    out_lane = lax.broadcasted_iota(jnp.int32, (rows, 2 * HEAD_DIM), 1)

    def step(src, state, masked):
        peak, acc = state
        scores = lax.dot_general(
            queries, k_aug[src], (((1,), (1,)), ((), ())), preferred_element_type=jnp.float32
        )
        if masked:
            row = lax.broadcasted_iota(jnp.int32, (rows, 1), 0)
            pos = row // sub * rows_dev + rank * sub + row % sub
            key = lo + lax.broadcasted_iota(jnp.int32, (1, count), 1)
            scores = jnp.where(key <= pos, scores, MASKED)
        new_peak = jnp.maximum(peak, jnp.max(scores, axis=1, keepdims=True))
        probs = jnp.exp(scores - new_peak).astype(jnp.bfloat16)
        acc = acc * jnp.exp(peak - new_peak) + jnp.dot(
            probs, v_aug[src], preferred_element_type=jnp.float32
        )
        return new_peak, acc

    if begun:
        before = state_ref[...]
        state = (before[:, 1:2], jnp.where(out_lane == 1, 0.0, before))
    else:
        state = (
            jnp.full((rows, 1), MASKED, jnp.float32),
            jnp.zeros((rows, 2 * HEAD_DIM), jnp.float32),
        )
    state = lax.fori_loop(0, tile, lambda i, state: step(i, state, False), state)
    peak, acc = step(tile, state, True)
    if not begun:
        o_ref[...] = jnp.where(out_lane == 1, peak, acc)
        return
    out = acc[:, HEAD_DIM:] / acc[:, :1]
    half = sub // 2
    for t in range(n_tp):
        top, low = (out[t * sub + step : t * sub + step + half] for step in (0, half))
        o_ref[t] = jnp.concatenate((top, low), axis=1).astype(o_ref.dtype)


def flash(got, kv, side_q, side_k, state, span, first, sub, rows_dev, n_tp, shares):
    n_sp, count = kv.shape[0], span[1] - span[0]
    chunk = n_tp * sub
    lanes = 2 * HEAD_DIM
    whole = pl.BlockSpec(memory_space=pltpu.VMEM)
    begun = state is not None
    wide = pl.BlockSpec((chunk, lanes), lambda i: (i, 0))
    if begun:
        out_shape = jax.ShapeDtypeStruct((n_sp * n_tp, sub // 2, lanes), jnp.bfloat16)
        out_spec = pl.BlockSpec((n_tp, sub // 2, lanes), lambda i: (i, 0, 0))
    else:
        out_shape = jax.ShapeDtypeStruct((n_sp * chunk, lanes), jnp.float32)
        out_spec = wide
    first_q = first // (chunk // 2)
    body = functools.partial(
        flash_kernel,
        begun=begun,
        span=span,
        shares=shares,
        sub=sub,
        rows_dev=rows_dev,
        n_tp=n_tp,
    )
    q_spec = pl.BlockSpec((1, chunk // 2, lanes), lambda i: (i, first_q, 0))
    pairs = n_sp * (n_sp + 1) // 2 * chunk * count
    return pl.pallas_call(
        body,
        grid=(n_sp,),
        out_shape=out_shape,
        in_specs=[q_spec, whole, wide, whole] + [wide] * begun,
        out_specs=out_spec,
        scratch_shapes=[pltpu.VMEM((n_sp, count, lanes), jnp.bfloat16)] * 2,
        compiler_params=pltpu.CompilerParams(vmem_limit_bytes=50 * 2**20),
        cost_estimate=pl.CostEstimate(
            flops=8 * lanes * pairs, bytes_accessed=2**22, transcendentals=pairs
        ),
        name="flash",
    )(got, kv, side_q, side_k, *([state] if begun else []))


def local(
    queries,
    key_rows,
    value_rows,
    cum_gate,
    residual,
    out_weight,
    gain_mix,
    gain_pre,
    gain_post,
    route_ids,
    route_weight,
    w_gate,
    w_up,
    w_down,
):
    tok_dev, feature_width = queries.shape
    local_heads = feature_width // HEAD_DIM
    n_sp, n_tp = lax.axis_size("sp"), lax.axis_size("tp")
    shares = n_sp // local_heads
    rows_dev = residual.shape[0]
    sub = rows_dev // shares
    chunk = n_tp * sub
    half = chunk // 2
    first = tok_dev * 5 // 8 // half * half
    one, two = pack(queries, key_rows, value_rows, first, shares, n_tp)
    got = lax.all_to_all(one, "sp", split_axis=0, concat_axis=0, tiled=True)
    got, two = lax.optimization_barrier((got, two))
    got_two = lax.all_to_all(two, "sp", split_axis=0, concat_axis=0, tiled=True)

    me = lax.axis_index("sp")
    gate = lax.dynamic_index_in_dim(cum_gate, me // shares, 0, keepdims=False)
    gate_q = gate.reshape(n_sp * n_tp, shares, sub)
    gate_q = lax.dynamic_index_in_dim(gate_q, me % shares, 1, keepdims=False).reshape(-1)
    ones_q = jnp.ones((n_sp * chunk,), jnp.bfloat16)
    ones_k = jnp.ones((n_sp * tok_dev,), jnp.bfloat16)
    side_q = jnp.stack(bf16_parts(gate_q) + [ones_q] * 3, axis=1)
    side_k = jnp.stack([ones_k] * 3 + bf16_parts(-gate), axis=1)
    pad = ((0, 0), (HEAD_DIM, HEAD_DIM - 6))
    side_q = jnp.pad(side_q, pad)
    side_k = jnp.pad(side_k, pad).reshape(n_sp, tok_dev, 2 * HEAD_DIM)
    fixed = (first, sub, rows_dev, n_tp, shares)
    state = flash(got, got, side_q, side_k, None, (0, first), *fixed)
    out = flash(got, got_two, side_q, side_k, state, (first, tok_dev), *fixed)
    heads = lax.all_to_all(out, ("sp", "tp"), split_axis=0, concat_axis=0, tiled=True)
    head_rows = assemble(heads, shares, n_tp, local_heads)
    projected = jnp.dot(head_rows, out_weight, preferred_element_type=jnp.float32)
    stream = (residual.astype(jnp.float32) + rms_scale(projected, gain_mix)).astype(jnp.bfloat16)
    stream_wide = lax.optimization_barrier(stream).astype(jnp.float32)
    normed = rms_scale(stream_wide, gain_pre).astype(jnp.bfloat16)
    top_count = route_ids.shape[1]
    experts_all = n_sp * n_tp
    capacity = max(2, (4 * rows_dev * top_count + 3 * experts_all - 1) // (3 * experts_all))
    capacity = (capacity + 7) // 8 * 8
    flat_ids = route_ids.reshape(-1)
    item = lax.iota(jnp.int32, rows_dev * top_count)
    earlier = (item[None, :] < item[:, None]) & (flat_ids[None, :] == flat_ids[:, None])
    slot_index = flat_ids * capacity + jnp.sum(earlier.astype(jnp.int32), axis=1)
    slot_index = slot_index.reshape(rows_dev, top_count)
    slots_all = experts_all * capacity
    slot = lax.iota(jnp.int32, slots_all)
    place = sum((slot_index[:, k, None] == slot).astype(jnp.bfloat16) for k in range(top_count))
    outgoing = lax.dot_general(
        place, normed, (((0,), (0,)), ((), ())), preferred_element_type=jnp.float32
    ).astype(jnp.bfloat16)
    outgoing = outgoing.reshape(experts_all, capacity, -1)
    arrived = lax.all_to_all(outgoing, ("sp", "tp"), split_axis=0, concat_axis=0, tiled=True)
    flat_rows = arrived.reshape(slots_all, -1)
    gate_act = jnp.dot(flat_rows, w_gate[0], preferred_element_type=jnp.float32)
    up_act = jnp.dot(flat_rows, w_up[0], preferred_element_type=jnp.float32)
    hidden = (jax.nn.silu(gate_act) * up_act).astype(jnp.bfloat16)
    expert_out = jnp.dot(hidden, w_down[0], preferred_element_type=jnp.float32).astype(jnp.bfloat16)
    returned = lax.all_to_all(
        expert_out.reshape(experts_all, capacity, -1),
        ("sp", "tp"),
        split_axis=0,
        concat_axis=0,
        tiled=True,
    ).reshape(slots_all, -1)
    weigh = sum(
        jnp.where(slot_index[:, k, None] == slot, route_weight[:, k, None], 0.0)
        for k in range(top_count)
    )
    combined = sum(
        jnp.dot(part, returned, preferred_element_type=jnp.float32) for part in bf16_parts(weigh)
    )
    return (stream_wide + rms_scale(combined, gain_post)).astype(jnp.bfloat16)


def solution(mesh):
    return jax.shard_map(
        local,
        mesh=mesh,
        in_specs=(
            P("sp", "tp"),
            P("sp", "tp"),
            P("sp", "tp"),
            P("tp", None),
            P(("sp", "tp"), None),
            P(),
            P(),
            P(),
            P(),
            P(("sp", "tp"), None),
            P(("sp", "tp"), None),
            P(("sp", "tp"), None, None),
            P(("sp", "tp"), None, None),
            P(("sp", "tp"), None, None),
        ),
        out_specs=P(("sp", "tp"), None),
        check_vma=False,
    )
```

```python
import functools
import math

import jax
import jax.numpy as jnp
from jax import lax
from jax.experimental import pallas as pl
from jax.experimental.pallas import tpu as pltpu
from jax.sharding import PartitionSpec as P

HEAD_DIM = 64
NORM_EPS = 1e-06
MASKED = -1e30


def rms_scale(rows, gain):
    mean_sq = jnp.mean(rows * rows, axis=-1, keepdims=True)
    return rows * lax.rsqrt(mean_sq + NORM_EPS) * gain


def bf16_parts(values):
    parts = []
    for _ in range(3):
        part = lax.reduce_precision(values, 8, 7)
        parts.append(part.astype(jnp.bfloat16))
        values = values - part
    return parts


def pack_kernel(q_ref, k_ref, v_ref, one_ref, two_ref, *, shares, n_tp):
    tok_dev, width = q_ref.shape
    first = tok_dev - two_ref.shape[1]
    rows_dev = tok_dev // n_tp
    sub = rows_dev // shares
    for h in range(width // HEAD_DIM):
        cols = pl.ds(h * HEAD_DIM, HEAD_DIM)
        pairs = jnp.concatenate((k_ref[:, cols], v_ref[:, cols]), axis=1)
        for r in range(shares):
            dest = h * shares + r
            one_ref[dest, :first] = pairs[:first]
            two_ref[dest] = pairs[first:]
            for t in range(n_tp // 2):
                low, high = (
                    q_ref[pl.ds((t + step) * rows_dev + r * sub, sub), cols]
                    for step in (0, n_tp // 2)
                )
                one_ref[dest, pl.ds(first + t * sub, sub)] = jnp.concatenate((low, high), axis=1)


def pack(queries, key_rows, value_rows, first, shares, n_tp):
    tok_dev, width = queries.shape
    dests = width // HEAD_DIM * shares
    half = tok_dev // shares // 2
    shapes = [(dests, first + half, 2 * HEAD_DIM), (dests, tok_dev - first, 2 * HEAD_DIM)]
    return pl.pallas_call(
        functools.partial(pack_kernel, shares=shares, n_tp=n_tp),
        out_shape=[jax.ShapeDtypeStruct(shape, jnp.bfloat16) for shape in shapes],
        in_specs=[pl.BlockSpec(memory_space=pltpu.VMEM)] * 3,
        out_specs=[pl.BlockSpec(memory_space=pltpu.VMEM)] * 2,
        compiler_params=pltpu.CompilerParams(vmem_limit_bytes=32 * 2**20),
        name="pack",
    )(queries, key_rows, value_rows)


def assemble_kernel(in_ref, out_ref, *, shares, n_tp, local_heads):
    half = in_ref.shape[1]
    for t in range(n_tp):
        for h in range(0, local_heads, 2):
            for r in range(shares):
                left = in_ref[(h * shares + r) * n_tp + t]
                right = in_ref[((h + 1) * shares + r) * n_tp + t]
                for part in range(2):
                    cols = slice(part * HEAD_DIM, (part + 1) * HEAD_DIM)
                    out_ref[
                        pl.ds((2 * r + part) * half, half),
                        pl.ds((t * local_heads + h) * HEAD_DIM, 2 * HEAD_DIM),
                    ] = jnp.concatenate((left[:, cols], right[:, cols]), axis=1)


def assemble(heads, shares, n_tp, local_heads):
    shape = (2 * shares * heads.shape[1], n_tp * local_heads * HEAD_DIM)
    return pl.pallas_call(
        functools.partial(
            assemble_kernel, shares=shares, n_tp=n_tp, local_heads=local_heads
        ),
        out_shape=jax.ShapeDtypeStruct(shape, jnp.bfloat16),
        in_specs=[pl.BlockSpec(memory_space=pltpu.VMEM)],
        out_specs=pl.BlockSpec(memory_space=pltpu.VMEM),
        name="assemble",
    )(heads)


def flash_kernel(*refs, begun, span, shares, sub, rows_dev, n_tp):
    if begun:
        q_ref, kv_ref, side_q_ref, side_k_ref, state_ref, o_ref, k_aug, v_aug = refs
    else:
        q_ref, kv_ref, side_q_ref, side_k_ref, o_ref, k_aug, v_aug = refs
    lo, hi = span
    count = hi - lo
    tile = pl.program_id(0)
    rank = lax.rem(lax.axis_index("sp"), shares)

    @pl.when(tile == 0)
    def _():
        lane = lax.broadcasted_iota(jnp.int32, (count, 2 * HEAD_DIM), 1)

        def one(src, carry):
            kv = kv_ref[src, :count].astype(jnp.float32)
            side = side_k_ref[src, lo:hi].astype(jnp.float32)
            k_aug[src] = jnp.where(lane < HEAD_DIM, kv, side).astype(jnp.bfloat16)
            ones = (lane == 0).astype(jnp.float32)
            v_aug[src] = jnp.where(lane < HEAD_DIM, ones, kv).astype(jnp.bfloat16)
            return carry

        lax.fori_loop(0, kv_ref.shape[0], one, 0)

    packed = q_ref[0]
    queries = jnp.concatenate((packed[:, :HEAD_DIM], packed[:, HEAD_DIM:]), axis=0)
    queries = queries * jnp.bfloat16(HEAD_DIM**-0.5)
    queries = jnp.concatenate((queries, side_q_ref[:, HEAD_DIM:]), axis=1)
    rows = queries.shape[0]
    out_lane = lax.broadcasted_iota(jnp.int32, (rows, 2 * HEAD_DIM), 1)

    def step(src, state, masked):
        peak, acc = state
        scores = lax.dot_general(
            queries, k_aug[src], (((1,), (1,)), ((), ())), preferred_element_type=jnp.float32
        )
        if masked:
            row = lax.broadcasted_iota(jnp.int32, (rows, 1), 0)
            pos = row // sub * rows_dev + rank * sub + row % sub
            key = lo + lax.broadcasted_iota(jnp.int32, (1, count), 1)
            scores = jnp.where(key <= pos, scores, MASKED)
        new_peak = jnp.maximum(peak, jnp.max(scores, axis=1, keepdims=True))
        probs = jnp.exp(scores - new_peak).astype(jnp.bfloat16)
        acc = acc * jnp.exp(peak - new_peak) + jnp.dot(
            probs, v_aug[src], preferred_element_type=jnp.float32
        )
        return new_peak, acc

    if begun:
        before = state_ref[...]
        kept = jnp.max(jnp.where(out_lane == 1, before, -jnp.inf), axis=1, keepdims=True)
        state = (kept, jnp.where(out_lane == 1, 0.0, before))
    else:
        state = (
            jnp.full((rows, 1), MASKED, jnp.float32),
            jnp.zeros((rows, 2 * HEAD_DIM), jnp.float32),
        )
    state = lax.fori_loop(0, tile, lambda i, state: step(i, state, False), state)
    peak, acc = step(tile, state, True)
    if not begun:
        o_ref[...] = jnp.where(out_lane == 1, peak, acc)
        return
    out = acc[:, HEAD_DIM:] / acc[:, :1]
    half = sub // 2
    for t in range(n_tp):
        top, low = (out[t * sub + step : t * sub + step + half] for step in (0, half))
        o_ref[t] = jnp.concatenate((top, low), axis=1).astype(o_ref.dtype)


def flash(got, kv, side_q, side_k, state, span, first, sub, rows_dev, n_tp, shares):
    n_sp, count = kv.shape[0], span[1] - span[0]
    chunk = n_tp * sub
    lanes = 2 * HEAD_DIM
    whole = pl.BlockSpec(memory_space=pltpu.VMEM)
    begun = state is not None
    wide = pl.BlockSpec((chunk, lanes), lambda i: (i, 0))
    if begun:
        out_shape = jax.ShapeDtypeStruct((n_sp * n_tp, sub // 2, lanes), jnp.bfloat16)
        out_spec = pl.BlockSpec((n_tp, sub // 2, lanes), lambda i: (i, 0, 0))
    else:
        out_shape = jax.ShapeDtypeStruct((n_sp * chunk, lanes), jnp.float32)
        out_spec = wide
    first_q = first // (chunk // 2)
    body = functools.partial(
        flash_kernel,
        begun=begun,
        span=span,
        shares=shares,
        sub=sub,
        rows_dev=rows_dev,
        n_tp=n_tp,
    )
    q_spec = pl.BlockSpec((1, chunk // 2, lanes), lambda i: (i, first_q, 0))
    pairs = n_sp * (n_sp + 1) // 2 * chunk * count
    return pl.pallas_call(
        body,
        grid=(n_sp,),
        out_shape=out_shape,
        in_specs=[q_spec, whole, wide, whole] + [wide] * begun,
        out_specs=out_spec,
        scratch_shapes=[pltpu.VMEM((n_sp, count, lanes), jnp.bfloat16)] * 2,
        compiler_params=pltpu.CompilerParams(vmem_limit_bytes=50 * 2**20),
        cost_estimate=pl.CostEstimate(
            flops=8 * lanes * pairs, bytes_accessed=2**22, transcendentals=pairs
        ),
        name="flash",
    )(got, kv, side_q, side_k, *([state] if begun else []))


def local(
    queries,
    key_rows,
    value_rows,
    cum_gate,
    residual,
    out_weight,
    gain_mix,
    gain_pre,
    gain_post,
    route_ids,
    route_weight,
    w_gate,
    w_up,
    w_down,
):
    tok_dev, feature_width = queries.shape
    local_heads = feature_width // HEAD_DIM
    n_sp, n_tp = lax.axis_size("sp"), lax.axis_size("tp")
    shares = n_sp // local_heads
    rows_dev = residual.shape[0]
    sub = rows_dev // shares
    chunk = n_tp * sub
    half = chunk // 2
    first = tok_dev * 5 // 8 // half * half
    one, two = pack(queries, key_rows, value_rows, first, shares, n_tp)
    got = lax.all_to_all(one, "sp", split_axis=0, concat_axis=0, tiled=True)
    got, two = lax.optimization_barrier((got, two))
    got_two = lax.all_to_all(two, "sp", split_axis=0, concat_axis=0, tiled=True)

    me = lax.axis_index("sp")
    gate = lax.dynamic_index_in_dim(cum_gate, me // shares, 0, keepdims=False)
    gate_q = gate.reshape(n_sp * n_tp, shares, sub)
    gate_q = lax.dynamic_index_in_dim(gate_q, me % shares, 1, keepdims=False).reshape(-1)
    ones_q = jnp.ones((n_sp * chunk,), jnp.bfloat16)
    ones_k = jnp.ones((n_sp * tok_dev,), jnp.bfloat16)
    lanes = jnp.arange(2 * HEAD_DIM)
    place_side = (lanes == HEAD_DIM + jnp.arange(6)[:, None]).astype(jnp.bfloat16)

    def side_lanes(parts):
        return lax.dot_general(
            jnp.stack(parts), place_side, (((0,), (0,)), ((), ())), preferred_element_type=jnp.float32
        ).astype(jnp.bfloat16)

    side_q = side_lanes(bf16_parts(gate_q) + [ones_q] * 3)
    side_k = side_lanes([ones_k] * 3 + bf16_parts(-gate))
    side_k = side_k.reshape(n_sp, tok_dev, 2 * HEAD_DIM)
    fixed = (first, sub, rows_dev, n_tp, shares)
    state = flash(got, got, side_q, side_k, None, (0, first), *fixed)
    out = flash(got, got_two, side_q, side_k, state, (first, tok_dev), *fixed)
    heads = lax.all_to_all(out, ("sp", "tp"), split_axis=0, concat_axis=0, tiled=True)
    head_rows = assemble(heads, shares, n_tp, local_heads)
    projected = jnp.dot(head_rows, out_weight, preferred_element_type=jnp.float32)
    stream = (residual.astype(jnp.float32) + rms_scale(projected, gain_mix)).astype(jnp.bfloat16)
    stream_wide = lax.optimization_barrier(stream).astype(jnp.float32)
    normed = rms_scale(stream_wide, gain_pre).astype(jnp.bfloat16)
    top_count = route_ids.shape[1]
    experts_all = n_sp * n_tp
    capacity = max(2, (4 * rows_dev * top_count + 3 * experts_all - 1) // (3 * experts_all))
    capacity = (capacity + 7) // 8 * 8
    flat_ids = route_ids.reshape(-1)
    item = lax.iota(jnp.int32, rows_dev * top_count)
    earlier = (item[None, :] < item[:, None]) & (flat_ids[None, :] == flat_ids[:, None])
    slot_index = flat_ids * capacity + jnp.sum(earlier.astype(jnp.int32), axis=1)
    slot_index = slot_index.reshape(rows_dev, top_count)
    slots_all = experts_all * capacity
    slot = lax.iota(jnp.int32, slots_all)
    place = sum((slot_index[:, k, None] == slot).astype(jnp.bfloat16) for k in range(top_count))
    outgoing = lax.dot_general(
        place, normed, (((0,), (0,)), ((), ())), preferred_element_type=jnp.float32
    ).astype(jnp.bfloat16)
    outgoing = outgoing.reshape(experts_all, capacity, -1)
    arrived = lax.all_to_all(outgoing, ("sp", "tp"), split_axis=0, concat_axis=0, tiled=True)
    flat_rows = arrived.reshape(slots_all, -1)
    gate_act = jnp.dot(flat_rows, w_gate[0], preferred_element_type=jnp.float32)
    up_act = jnp.dot(flat_rows, w_up[0], preferred_element_type=jnp.float32)
    hidden = (jax.nn.silu(gate_act) * up_act).astype(jnp.bfloat16)
    expert_out = jnp.dot(hidden, w_down[0], preferred_element_type=jnp.float32).astype(jnp.bfloat16)
    returned = lax.all_to_all(
        expert_out.reshape(experts_all, capacity, -1),
        ("sp", "tp"),
        split_axis=0,
        concat_axis=0,
        tiled=True,
    ).reshape(slots_all, -1)
    weigh = sum(
        jnp.where(slot_index[:, k, None] == slot, route_weight[:, k, None], 0.0)
        for k in range(top_count)
    )
    combined = sum(
        jnp.dot(part, returned, preferred_element_type=jnp.float32) for part in bf16_parts(weigh)
    )
    return (stream_wide + rms_scale(combined, gain_post)).astype(jnp.bfloat16)


def solution(mesh):
    return jax.shard_map(
        local,
        mesh=mesh,
        in_specs=(
            P("sp", "tp"),
            P("sp", "tp"),
            P("sp", "tp"),
            P("tp", None),
            P(("sp", "tp"), None),
            P(),
            P(),
            P(),
            P(),
            P(("sp", "tp"), None),
            P(("sp", "tp"), None),
            P(("sp", "tp"), None, None),
            P(("sp", "tp"), None, None),
            P(("sp", "tp"), None, None),
        ),
        out_specs=P(("sp", "tp"), None),
        check_vma=False,
    )
```
